32 devices in a mesh: ep: 16 (over z, y, x), tp: 2 (over core).
Axes of the slice: x: 2, y: 2, z: 4, core: 2. Of those that a mesh axis runs over, the one named last changes fastest.
Arguments:
- tokens: bfloat16 [2048, 2048], P('ep'), may hold values from -6 to 6
- expert_ids: int32 [2048, 2], P('ep'), may hold values from 0 to 7, all different within a row; in each aligned block of 128 rows (0 to 127, 128 to 255, ...) at most 64 rows name the same one
- route_weights: float32 [2048, 2], P('ep'), may hold values from 0.2 to 1
- norm_gain: float32 [2048], replicated, may hold values from 0.1 to 1.9
- gate_weight: bfloat16 [2048, 8192], P(None, ('ep', 'tp')), may hold values from -0.125 to 0.125
- up_weight: bfloat16 [2048, 8192], P(None, ('ep', 'tp')), may hold values from -0.125 to 0.125
- down_weight: bfloat16 [8192, 2048], P('ep', 'tp'), may hold values from -0.1875 to 0.1875
- dense_gate: bfloat16 [2048, 256], P('ep'), may hold values from -0.125 to 0.125
- dense_up: bfloat16 [2048, 256], P('ep'), may hold values from -0.125 to 0.125
- dense_down: bfloat16 [256, 2048], P(None, 'tp'), may hold values from -0.375 to 0.375
- branch_gate: float32 [2048], P('tp'), may hold values from -3 to 3
Outputs:
- mixed: bfloat16 [2048, 2048], P('ep', 'tp')
The draws below stay inside these ranges and needn't reach their ends.
Inputs may be any that keep to these rules, and one draw needn't show every extreme that they name: `expert_ids`: each row names 2 different experts. Within the rows of one device (aligned blocks of 128 rows) no expert is named more than 64 times; in some blocks an expert is named exactly 64 times.
All inputs are finite; a program needn't handle non-finite values.
Results may differ from the reference program's by a relative error of at most 0.0074.
Values may be sent and summed in bfloat16 or wider, within the bound.
A program may use at most 64 MiB of HBM per device.

```python
import math
import jax
import jax.numpy as jnp
import numpy as np
from jax import lax

D = 2048
FF = 1024
SH = 256
TOP = 2
TOK_DEV = 128
EXPERTS = 8
TOKENS = 2048
SLOTS = 64
N_EP = 16


def levels(stream_key, dims, pieces, least, top_value):
    loudness, own = 1.0, jax.random.fold_in(stream_key, 6)
    for dim, blocks in pieces:
        heights = jnp.exp(jax.random.uniform(jax.random.fold_in(own, dim), (blocks,), jnp.float32, least / len(pieces), top_value / len(pieces)))
        loudness = loudness * jnp.repeat(heights, dims[dim] // blocks).reshape([-1 if axis == dim else 1 for axis in range(len(dims))])
    return loudness


def deal_out(key, own, number, rows, count, top, limit, skew):
    order = jax.random.permutation(key, count)
    crowded, common = portions_of(count, rows * top, limit, skew, True), portions_of(count, rows * top, limit, skew, False)
    places = jnp.arange(count)

    def named(tallies, rotation):
        used = int((tallies > 0).sum())
        fixed = max(1, used // 4)
        passed = fixed + (places - fixed + rotation * (used - fixed)) % max(1, count - fixed)
        return jnp.zeros((count,), jnp.int32).at[order[jnp.where(places < fixed, places, passed)]].set(jnp.asarray(tallies, jnp.int32))

    tallies = jnp.where(number % 4 == 0, named(crowded, number // 4), named(common, number - number // 4 - 1))
    mixed = jax.random.permutation(jax.random.fold_in(own, 3), count)
    source_of, taker = mixed[0:count // 2 * 2:2], mixed[1:count // 2 * 2:2]
    room = jnp.minimum(tallies[source_of] - 1, limit - tallies[taker]) // 2
    room = jnp.where((source_of == order[0]) | (taker == order[0]) | (tallies[taker] == 0), 0, jnp.maximum(room, 0))
    passed = jax.random.randint(jax.random.fold_in(own, 4), (count // 2,), 0, 1 << 20) % (room + 1)
    tallies = tallies.at[source_of].add(-passed).at[taker].add(passed)
    items = jnp.searchsorted(jnp.cumsum(tallies), jnp.arange(rows * top), side="right").astype(jnp.int32)
    table = items.reshape(top, rows).T
    table = table[jax.random.permutation(jax.random.fold_in(own, 1), rows)]
    rotation = jax.random.randint(jax.random.fold_in(own, 2), (rows, 1), 0, top)
    return jnp.take_along_axis(table, (jnp.arange(top)[None, :] + rotation) % top, axis=1)


def portions_of(number_of, total, bound, lean, full):
    weights = [(1 << 20) // math.isqrt(grade ** lean) + 1 for grade in range(1, number_of + 1)]
    largest = bound if full else min(bound, max(-(-total // number_of), total * weights[0] // sum(weights)))
    least = 1 if total - largest >= number_of - 1 else 0
    given, spare = [largest] + [least] * (number_of - 1), total - largest - least * (number_of - 1)
    while spare > 0:
        candidates = [i for i in range(1, number_of) if given[i] < largest] or [i for i in range(1, number_of) if given[i] < bound]
        pool, remaining = sum([weights[i] for i in candidates]), spare
        for i in candidates:
            extra = min(bound - given[i], max(1, remaining * weights[i] // pool), spare)
            given[i] = given[i] + extra
            spare = spare - extra
    return np.array(given)


def noise(own_key, shape, width, reach, pieces=(), kind=jnp.bfloat16):
    drawn = width * jax.random.normal(own_key, shape, jnp.float32)
    if pieces:
        drawn = drawn * levels(own_key, shape, pieces, -0.22, 0.18)
    return jnp.clip(drawn, -reach, reach).astype(kind)


def setup_inputs(seed: int = 0) -> dict:
    keys = jax.random.split(jax.random.key(seed), 12)
    tokens = noise(keys[0], (TOKENS, D), 1.0, 6.0, ((0, 16),))
    expert_ids_keys = jax.random.split(jax.random.fold_in(keys[1], 1), TOKENS // TOK_DEV)
    expert_ids_turns = jax.random.permutation(jax.random.fold_in(keys[1], 3), TOKENS // TOK_DEV)
    expert_ids = jax.vmap(lambda own, number: deal_out(jax.random.fold_in(keys[1], 2), own, number, TOK_DEV, EXPERTS, TOP, SLOTS, 2))(expert_ids_keys, expert_ids_turns).reshape((TOKENS, TOP))
    route_weights = jnp.clip(0.2 + 0.8 * jax.random.uniform(keys[2], (TOKENS, TOP), jnp.float32) ** levels(keys[2], (TOKENS, TOP), ((0, 16),), -0.2, 0.2), 0.2, 1.0)
    norm_gain = jnp.clip(1.0 + 0.18 * jax.random.normal(keys[3], (D,), jnp.float32), 0.1, 1.9)
    gate_weight = noise(keys[4], (D, EXPERTS * FF), D ** -0.5, 0.125, ((1, 32),))
    up_weight = noise(keys[5], (D, EXPERTS * FF), D ** -0.5, 0.125, ((1, 32),))
    down_weight = noise(keys[6], (EXPERTS * FF, D), FF ** -0.5, 0.1875, ((0, 16), (1, 2)))
    dense_gate = noise(keys[7], (D, SH), D ** -0.5, 0.125, ((0, 16),))
    dense_up = noise(keys[8], (D, SH), D ** -0.5, 0.125, ((0, 16),))
    dense_down = noise(keys[9], (SH, D), SH ** -0.5, 0.375, ((1, 2),))
    branch_gate = jnp.clip(jax.random.uniform(keys[10], (D,), jnp.float32, -3.0, 3.0) * levels(keys[10], (D,), ((0, 2),), -0.4, 0.0), -3.0, 3.0)
    return dict(tokens=tokens, expert_ids=expert_ids, route_weights=route_weights, norm_gain=norm_gain, gate_weight=gate_weight, up_weight=up_weight, down_weight=down_weight, dense_gate=dense_gate, dense_up=dense_up, dense_down=dense_down, branch_gate=branch_gate)


epsilon = 1e-06

def reference(tokens, expert_ids, route_weights, norm_gain, gate_weight, up_weight, down_weight, dense_gate, dense_up, dense_down, branch_gate):
    model_width = tokens.shape[1]
    values = tokens.astype(jnp.float32)
    inverse = lax.rsqrt(lax.optimization_barrier(jnp.mean(values * values, axis=1, keepdims=True)) + epsilon)
    normed = (values * inverse * norm_gain[None, :]).astype(jnp.bfloat16)
    dense_gate_act = jnp.dot(normed, dense_gate, preferred_element_type=jnp.float32)
    dense_up_act = jnp.dot(normed, dense_up, preferred_element_type=jnp.float32)
    dense_hidden = (jax.nn.silu(dense_gate_act) * dense_up_act).astype(jnp.bfloat16)
    dense_out = jnp.dot(dense_hidden, dense_down, preferred_element_type=jnp.float32)
    flat_ids = expert_ids.reshape(N_EP, TOK_DEV * TOP)
    labels = jnp.arange(EXPERTS, dtype=jnp.int32)
    onehot = (flat_ids[:, :, None] == labels[None, None, :]).astype(jnp.int32)
    earlier = jnp.cumsum(onehot, axis=1) - onehot
    slot_index = lax.optimization_barrier(jnp.sum(onehot * earlier, axis=2)).astype(jnp.int32)
    source = jnp.arange(N_EP, dtype=jnp.int32)[:, None]
    slot_row = (source * SLOTS + slot_index).astype(jnp.int32)
    owner_rows = (jnp.arange(TOK_DEV * TOP, dtype=jnp.int32)[None, :] // TOP + source * TOK_DEV).astype(jnp.int32)
    row_table = jnp.full((EXPERTS, N_EP * SLOTS), TOKENS, jnp.int32)
    row_table = row_table.at[flat_ids.reshape(-1), slot_row.reshape(-1)].set(owner_rows.reshape(-1))
    padded = jnp.concatenate([normed, jnp.zeros((1, model_width), jnp.bfloat16)], axis=0)
    half_width = FF // 2

    def run_expert(expert_index):
        in_rows = padded[row_table[expert_index]]
        offset = (expert_index * FF).astype(jnp.int32)
        w_gate = lax.dynamic_slice_in_dim(gate_weight, offset, FF, 1)
        w_up = lax.dynamic_slice_in_dim(up_weight, offset, FF, 1)
        w_down = lax.dynamic_slice_in_dim(down_weight, offset, FF, 0)
        expert_gate = jnp.dot(in_rows, w_gate, preferred_element_type=jnp.float32)
        expert_up = jnp.dot(in_rows, w_up, preferred_element_type=jnp.float32)
        hidden = (jax.nn.silu(expert_gate) * expert_up).astype(jnp.bfloat16)
        lower_part = jnp.dot(hidden[:, :half_width], w_down[:half_width], preferred_element_type=jnp.float32).astype(jnp.bfloat16)
        upper_part = jnp.dot(hidden[:, half_width:], w_down[half_width:], preferred_element_type=jnp.float32).astype(jnp.bfloat16)
        return (lower_part.astype(jnp.float32) + upper_part.astype(jnp.float32)).astype(jnp.bfloat16)
    results = lax.map(run_expert, jnp.arange(EXPERTS, dtype=jnp.int32))
    picked = results[flat_ids.reshape(TOKENS, TOP), slot_row.reshape(TOKENS, TOP)]
    routed = lax.optimization_barrier(jnp.sum(route_weights[:, :, None] * picked.astype(jnp.float32), axis=1))
    mixed_out = routed + jax.nn.sigmoid(branch_gate)[None, :] * dense_out
    return mixed_out.astype(jnp.bfloat16)
```

```python
import functools

import jax
import jax.numpy as jnp
from jax import lax
from jax.experimental import pallas as pl
from jax.experimental.pallas import tpu as pltpu
from jax.sharding import PartitionSpec as P

epsilon = 1e-06


def narrowed(rows):
    half_features = rows.shape[2] // 2
    return lax.dynamic_slice_in_dim(rows, lax.axis_index("tp") * half_features, half_features, 2)


def small_slot_path(
    tokens,
    expert_ids,
    route_weights,
    norm_gain,
    gate_weight,
    up_weight,
    down_weight,
    dense_gate,
    dense_up,
    dense_down,
    branch_gate,
):
    tok_rows, model_width = tokens.shape
    top_count = expert_ids.shape[1]
    ep_count = lax.axis_size("ep")
    experts = ep_count // 2
    slot_count = 2 * top_count * tok_rows // experts
    values = tokens.astype(jnp.float32)
    inverse = lax.rsqrt(jnp.mean(values * values, axis=1, keepdims=True) + epsilon)
    normed = (values * inverse * norm_gain[None, :]).astype(jnp.bfloat16)
    dense_gate_act = jnp.dot(
        normed,
        lax.all_gather(dense_gate, "ep", axis=0, tiled=True),
        preferred_element_type=jnp.float32,
    )
    dense_up_act = jnp.dot(
        normed,
        lax.all_gather(dense_up, "ep", axis=0, tiled=True),
        preferred_element_type=jnp.float32,
    )
    dense_hidden = (jax.nn.silu(dense_gate_act) * dense_up_act).astype(jnp.bfloat16)
    dense_out = jnp.dot(dense_hidden, dense_down, preferred_element_type=jnp.float32)
    flat_ids = expert_ids.reshape(tok_rows * top_count)
    labels = lax.broadcasted_iota(jnp.int32, (1, experts), 1)
    onehot = (flat_ids[:, None] == labels).astype(jnp.int32)
    earlier = jnp.cumsum(onehot, axis=0) - onehot
    slot_index = jnp.sum(onehot * earlier, axis=1)
    row_code = (flat_ids * slot_count + slot_index).reshape(tok_rows, top_count)
    targets = lax.broadcasted_iota(jnp.int32, (experts * slot_count, 1, 1), 0)
    selector = jnp.any(row_code[None, :, :] == targets, axis=2).astype(jnp.bfloat16)
    buffer = jnp.dot(selector, normed, preferred_element_type=jnp.float32).astype(jnp.bfloat16)
    buffer = buffer.reshape(experts, slot_count, model_width)
    outgoing = narrowed(jnp.repeat(buffer, 2, axis=0))
    arrived = lax.all_gather(
        lax.all_to_all(outgoing, "ep", split_axis=0, concat_axis=0, tiled=True),
        "tp",
        axis=2,
        tiled=True,
    )
    in_rows = arrived.reshape(ep_count * slot_count, model_width)
    expert_gate = jnp.dot(in_rows, gate_weight, preferred_element_type=jnp.float32)
    expert_up = jnp.dot(in_rows, up_weight, preferred_element_type=jnp.float32)
    hidden = (jax.nn.silu(expert_gate) * expert_up).astype(jnp.bfloat16)
    down_total = jnp.dot(
        lax.all_gather(hidden, "tp", axis=1, tiled=True),
        down_weight,
        preferred_element_type=jnp.float32,
    )
    partial_value = down_total.astype(jnp.bfloat16).reshape(ep_count, slot_count, -1)
    returned_rows = lax.all_to_all(partial_value, "ep", split_axis=0, concat_axis=0, tiled=True)
    pair_sums = returned_rows.reshape(experts, 2, slot_count, -1).astype(jnp.float32)
    expert_out = (
        (pair_sums[:, 0] + pair_sums[:, 1]).astype(jnp.bfloat16).reshape(experts * slot_count, -1)
    )
    picked = (
        jnp.take(expert_out, row_code.reshape(-1), axis=0)
        .reshape(tok_rows, top_count, -1)
        .astype(jnp.float32)
    )
    routed = jnp.sum(route_weights[:, :, None] * picked, axis=1)
    mixed_out = routed + jax.nn.sigmoid(branch_gate)[None, :] * dense_out
    return mixed_out.astype(jnp.bfloat16)


MESH = pl.DeviceIdType.MESH
BF16, F32 = jnp.bfloat16, jnp.float32


def flip(value, bits):
    bit = 1
    while bit <= bits:
        if bits & bit:
            value = value + bit * (1 - 2 * lax.rem(lax.div(value, bit), 2))
        bit *= 2
    return value


PLANES, OWN_CHUNKS, CROSSED = 4, 2, 1
PLAN = (
    ("along", 0, 0),
    ("cross", 0, 0),
    ("along", 0, 1),
    ("scatter", 0, 0),
    ("take", 0, 0),
    ("take", 1, 0),
    ("along", 0, 2),
    ("along", 1, 0),
    ("over", 1, 0),
    ("take", 0, 1),
    ("take", 2, 0),
    ("take", 1, 1),
    ("take", 0, 2),
    ("share", 0, 0),
    ("along", 2, 0),
    ("spread_x", 0, 0),
    ("take", 1, 2),
    ("share", 1, 0),
    ("along", 1, 1),
    ("over", 0, 0),
    ("along", 2, 2),
    ("take", 2, 2),
    ("expand", 1, 0),
    ("over", 2, 0),
    ("along", 2, 1),
    ("take", 2, 1),
    ("share", 2, 0),
    ("contract", 1, 0),
    ("spread_y", 0, 0),
    ("expand", 2, 0),
    ("contract", 2, 0),
    ("along", 3, 0),
    ("share", 2, 1),
    ("along", 1, 2),
    ("take", 3, 0),
    ("along", 3, 1),
    ("share", 1, 1),
    ("take", 3, 1),
    ("expand", 2, 1),
    ("share", 0, 1),
    ("contract", 2, 1),
    ("along", 3, 2),
    ("reduce", 2, 0),
    ("expand", 1, 1),
    ("over", 3, 0),
    ("take", 3, 2),
    ("share", 3, 0),
    ("expand", 0, 1),
    ("dense_act", 0, 0),
    ("contract", 1, 1),
    ("contract", 0, 1),
    ("dense_back", 0, 0),
    ("reduce", 2, 1),
    ("share", 3, 1),
    ("reduce", 1, 0),
    ("expand", 3, 1),
    ("contract", 3, 1),
    ("reduce", 1, 1),
    ("expand", 0, 0),
    ("expand", 3, 0),
    ("contract", 3, 0),
    ("contract", 0, 0),
    ("reduce", 3, 1),
    ("reduce", 0, 1),
    ("reduce", 3, 0),
    ("reduce", 0, 0),
    ("dense_pair", 0, 0),
    ("dense_out", 0, 0),
    ("collect", 1, 0),
    ("collect", 2, 0),
    ("collect", 3, 0),
    ("collect", 0, 0),
)


def expert_kernel(
    dims,
    tokens_ref,
    ids_ref,
    route_ref,
    gain_ref,
    gate_hbm,
    up_hbm,
    down_hbm,
    dense_gate_hbm,
    dense_up_hbm,
    dense_down_hbm,
    branch_ref,
    out_ref,
    blocks,
    meta,
    rows_in,
    row_send,
    hidden,
    half_own,
    half_in,
    summed,
    returned,
    gate_w,
    up_w,
    down_w,
    dense_gate_v,
    dense_up_v,
    dense_down_v,
    slices,
    dense_w,
    act_part,
    act_in,
    dense_hid,
    dense_units,
    total,
    load_sem,
    meta_send,
    meta_recv,
    up_send,
    down_send,
    block_recv,
    cross_send,
    cross_recv,
    y_send,
    y_recv,
    x_send,
    x_recv,
    xy_send,
    xy_recv,
    core_send,
    core_recv,
    hid_send,
    hid_recv,
    half_send,
    half_recv,
    ret_send,
    ret_recv,
    slice_send,
    slice_recv,
    dense_send,
    dense_recv,
    back_send,
    back_recv,
):
    ep_count, experts, slot_count, top_count = dims
    tok_rows = tokens_ref.shape[0]
    chunk = blocks.shape[3]
    half_width = chunk * OWN_CHUNKS
    quarter = dense_gate_v.shape[1] // PLANES
    ep, tp = lax.axis_index("ep"), lax.axis_index("tp")
    other = 1 - tp
    side, line, plane = lax.rem(ep, 2), lax.rem(lax.div(ep, 2), 2), lax.div(ep, 4)
    inner = lax.rem(lax.div(plane + 1, 2), 2)
    near, far = flip(plane, 2), flip(plane, 3)
    rounds = [plane, flip(plane, 1), near + inner * (far - near), far + inner * (near - far)]

    def place(to_plane, to_line=None, to_side=None, core=None):
        to_line = line if to_line is None else to_line
        to_side = side if to_side is None else to_side
        return (4 * to_plane + 2 * to_line + to_side, tp if core is None else core)

    across_x = place(plane, None, 1 - side)
    across_y = place(plane, 1 - line)
    across_core = place(plane, None, None, other)

    def remote(src, dst, send, recv, device):
        return pltpu.make_async_remote_copy(
            src_ref=src, dst_ref=dst, send_sem=send, recv_sem=recv,
            device_id=device, device_id_type=MESH,
        )

    barrier = pltpu.get_barrier_semaphore()
    greeted = [across_x, across_core, across_y]
    for other_plane in rounds[1:]:
        greeted += [place(other_plane), place(other_plane, 1 - line)]
    for device in greeted:
        pl.semaphore_signal(barrier, inc=1, device_id=device, device_id_type=MESH)

    dense_depth = dense_down_hbm.shape[0]
    loads = [
        pltpu.make_async_copy(source, target, load_sem.at[i])
        for i, (source, target) in enumerate(
            (
                (dense_gate_hbm, dense_gate_v),
                (dense_up_hbm, dense_up_v),
                (dense_down_hbm, dense_down_v.at[pl.ds(0, dense_depth)]),
                (gate_hbm, gate_w),
                (up_hbm, up_w),
                (down_hbm, down_w),
            )
        )
    ]
    for load in loads:
        load.start()

    values = tokens_ref[...].astype(F32)
    inverse = lax.rsqrt(jnp.mean(values * values, axis=1, keepdims=True) + epsilon)
    for i in range(OWN_CHUNKS):
        columns = pl.ds(pl.multiple_of(tp * half_width + i * chunk, chunk), chunk)
        blocks[plane, i] = (
            tokens_ref[:, columns].astype(F32) * inverse * gain_ref[:, columns]
        ).astype(BF16)

    def iota(shape, axis):
        return lax.broadcasted_iota(jnp.int32, shape, axis)

    label_rows = max(experts, 16)
    labels = iota((label_rows, tok_rows), 0)
    hits = [ids_ref[t : t + 1, :] == labels for t in range(top_count)]
    named = sum(hit.astype(F32) for hit in hits).astype(BF16)
    before = (iota((tok_rows, tok_rows), 0) < iota((tok_rows, tok_rows), 1)).astype(F32)
    earlier = jnp.dot(named, before.astype(BF16), preferred_element_type=F32)
    meta_rows = iota((meta.shape[2], tok_rows), 0)
    code_rows = iota((8, tok_rows), 0)
    listed = jnp.zeros(meta_rows.shape, F32)
    coded = jnp.zeros(code_rows.shape, F32)
    for t in range(top_count):
        expert = ids_ref[t : t + 1, :].astype(F32)
        slot = jnp.sum(jnp.where(hits[t], earlier, 0.0), axis=0, keepdims=True)
        listed = jnp.where(meta_rows == 2 * t, expert, listed)
        listed = jnp.where(meta_rows == 2 * t + 1, slot, listed)
        coded = jnp.where(code_rows == t, expert * slot_count + slot, coded)
    meta[plane, 0] = listed.astype(BF16)
    codes = jnp.transpose(coded)
    shares = jnp.transpose(route_ref[...])

    pl.semaphore_wait(barrier, len(greeted))

    unsent = []

    def send(copy, condition=None):
        unsent.append((copy, condition))
        if condition is None:
            copy.start()
        else:
            pl.when(condition)(copy.start)

    seen = set()

    def arrived(key, ref, send_sem, recv_sem, condition=None):
        if key in seen:
            return
        seen.add(key)
        copy = remote(ref, ref, send_sem, recv_sem, across_core)
        if condition is None:
            copy.wait_recv()
        else:
            pl.when(condition)(copy.wait_recv)

    plain = OWN_CHUNKS - CROSSED
    parts = OWN_CHUNKS + CROSSED

    def belongs(i):
        return (0, i) if i < OWN_CHUNKS else (1, i - CROSSED)

    def cross(_, j):
        if j == 0:
            send(
                remote(
                    meta.at[plane, 0], meta.at[plane, 1],
                    meta_send.at[0, 0], meta_recv.at[plane, 1], across_x,
                )
            )
        send(
            remote(
                blocks.at[plane, plain + j], blocks.at[plane, OWN_CHUNKS + j],
                cross_send.at[j], cross_recv.at[j], across_x,
            )
        )

    def have(r, i):
        z = rounds[r]
        if r == 0:
            if i >= OWN_CHUNKS:
                arrived(("meta", r, 1), meta.at[z, 1], meta_send.at[0, 0], meta_recv.at[z, 1])
                j = i - OWN_CHUNKS
                arrived(("cross", j), blocks.at[z, i], cross_send.at[j], cross_recv.at[j])
            return
        of = belongs(i)[0]
        arrived(("meta", r, of), meta.at[z, of], meta_send.at[0, 0], meta_recv.at[z, of])
        arrived(("block", r, i), blocks.at[z, i], up_send.at[r, i], block_recv.at[z, i])

    def along(r, i):
        have(r, i)
        z = rounds[r]
        of = belongs(i)[0]
        first = i in (0, OWN_CHUNKS)
        upward = (z <= plane) & (plane < PLANES - 1)
        downward = (z >= plane) & (plane > 0)
        ways = ((upward, jnp.minimum(plane + 1, PLANES - 1), up_send, 1),)
        ways += ((downward, jnp.maximum(plane - 1, 0), down_send, 2),)
        for condition, target, sems, m in ways:
            if first:
                piece = meta.at[z, of]
                send(
                    remote(
                        piece, piece, meta_send.at[m, 2 * r + of], meta_recv.at[z, of], place(target)
                    ),
                    condition,
                )
            piece = blocks.at[z, i]
            send(remote(piece, piece, sems.at[r, i], block_recv.at[z, i], place(target)), condition)

    pick_row = iota((2 * slot_count, tok_rows), 0)
    pick_expert = (
        2 * plane + jnp.where(pick_row < slot_count, line, 1 - line)
    ).astype(F32)
    pick_slot = jnp.bitwise_and(pick_row, slot_count - 1).astype(F32)

    def take(r, i):
        have(r, i)
        z = rounds[r]
        of, c = belongs(i)
        listing = meta[z, of].astype(F32)
        chosen = sum(
            (
                (listing[2 * t : 2 * t + 1] == pick_expert)
                & (listing[2 * t + 1 : 2 * t + 2] == pick_slot)
            ).astype(F32)
            for t in range(top_count)
        ).astype(BF16)
        picked = jnp.dot(chosen, blocks[z, i], preferred_element_type=F32).astype(BF16)
        rows_in[z, 0, tp, of, c] = picked[:slot_count]
        row_send[r, i] = picked[slot_count:]
        send(
            remote(
                row_send.at[r, i], rows_in.at[z, 1, tp, of, c],
                y_send.at[r, i], y_recv.at[z, i], across_y,
            )
        )
        if i < plain:
            send(
                remote(
                    rows_in.at[z, 0, tp, 0, i], rows_in.at[z, 0, tp, 1, i],
                    x_send.at[r, i], x_recv.at[z, i], across_x,
                )
            )

    def have_line(r, i):
        of, c = belongs(i)
        z = rounds[r]
        arrived(("y", r, i), rows_in.at[z, 1, tp, of, c], y_send.at[r, i], y_recv.at[z, i])

    def over(r, i):
        have_line(r, i)
        z = rounds[r]
        send(
            remote(
                rows_in.at[z, 1, tp, 0, i], rows_in.at[z, 1, tp, 1, i],
                xy_send.at[r, i], xy_recv.at[z, i], across_x,
            )
        )

    def share(r, g):
        z = rounds[r]
        if g:
            for i in range(parts):
                have_line(r, i)
        sems = ((x_send, x_recv), (xy_send, xy_recv))[g]
        for i in range(plain):
            arrived(
                ("x", r, g, i), rows_in.at[z, g, tp, 1, i], sems[0].at[r, i], sems[1].at[z, i]
            )
        piece = rows_in.at[z, g, tp]
        send(remote(piece, piece, core_send.at[r, g], core_recv.at[z, g], across_core))

    def expand(r, g):
        z = rounds[r]
        arrived(
            ("core", r, g), rows_in.at[z, g, other], core_send.at[r, g], core_recv.at[z, g]
        )
        if not loaded:
            for load in loads[3:]:
                load.wait()
            loaded.append(True)
        gate, up = 0.0, 0.0
        for core in range(2):
            for c in range(OWN_CHUNKS):
                rows = rows_in[z, g, core, :, c].reshape(2 * slot_count, chunk)
                depth = pl.ds((core * OWN_CHUNKS + c) * chunk, chunk)
                gate = gate + jnp.dot(rows, gate_w[depth, :], preferred_element_type=F32)
                up = up + jnp.dot(rows, up_w[depth, :], preferred_element_type=F32)
        hidden[z, g, tp] = (jax.nn.silu(gate) * up).astype(BF16)
        piece = hidden.at[z, g, tp]
        send(remote(piece, piece, hid_send.at[r, g], hid_recv.at[z, g], across_core))

    def contract(r, g):
        z = rounds[r]
        arrived(("hid", r, g), hidden.at[z, g, other], hid_send.at[r, g], hid_recv.at[z, g])
        units = jnp.concatenate([hidden[z, g, 0], hidden[z, g, 1]], axis=1)
        half_own[r, g] = (
            jnp.dot(units, down_w[...], preferred_element_type=F32)
            .astype(BF16)
            .reshape(2, slot_count, half_width)
        )
        send(
            remote(
                half_own.at[r, g, 1], half_in.at[z, g],
                half_send.at[r, g], half_recv.at[z, g], across_x,
            )
        )

    def reduce(r, g):
        z = rounds[r]
        arrived(("half", r, g), half_in.at[z, g], half_send.at[r, g], half_recv.at[z, g])
        result = (half_own[r, g, 0].astype(F32) + half_in[z, g].astype(F32)).astype(BF16)
        mine = 2 * plane + line
        if r == 0 and g == 0:
            returned[mine] = result
            return
        summed[r, g] = result
        target = place(z, 1 - line if g else line)
        send(remote(summed.at[r, g], returned.at[mine], ret_send.at[r, g], ret_recv.at[mine], target))

    half_plane = lax.rem(plane, 2)
    feeds = tp == lax.div(plane, 2)

    def scatter(r, g):
        loads[0].wait()
        loads[1].wait()
        lane = iota((dense_gate_v.shape[0], 2 * quarter), 1)
        for q in range(PLANES):
            columns = pl.ds((q // 2) * 2 * quarter, 2 * quarter)
            gate = dense_gate_v[:, columns].astype(F32)
            up = dense_up_v[:, columns].astype(F32)
            if q % 2:
                gate = pltpu.roll(gate, quarter, 1)
            else:
                up = pltpu.roll(up, quarter, 1)
            slices[q] = jnp.where(lane < quarter, gate, up).astype(BF16)

        @pl.when(feeds)
        def _():
            dense_w[line, side, half_plane] = slices[plane]

        for q in range(1, PLANES):
            z = rounds[q]
            send(
                remote(
                    slices.at[z], dense_w.at[line, side, half_plane],
                    slice_send.at[q], slice_recv.at[half_plane], place(z),
                ),
                feeds,
            )

    def spread_x(r, g):
        for h in range(2):
            arrived(
                ("slice", h), dense_w.at[line, side, h], slice_send.at[1], slice_recv.at[h],
                2 * tp + h != plane,
            )
        piece = dense_w.at[line, side]
        send(remote(piece, piece, dense_send.at[0], dense_recv.at[0], across_x))

    def spread_y(r, g):
        arrived(("wx",), dense_w.at[line, 1 - side], dense_send.at[0], dense_recv.at[0])
        piece = dense_w.at[line]
        send(remote(piece, piece, dense_send.at[1], dense_recv.at[1], across_y))

    def dense_act(r, g):
        arrived(("wy",), dense_w.at[1 - line], dense_send.at[1], dense_recv.at[1])
        weights = jnp.concatenate(
            [dense_w[l, s, h] for h in range(2) for l in range(2) for s in range(2)], axis=0
        )
        half_rows = tok_rows // 2
        for q in range(PLANES):
            act = 0.0
            for i in range(OWN_CHUNKS):
                have(q, i)
                act = act + jnp.dot(
                    blocks[rounds[q], i], weights[i * chunk : (i + 1) * chunk],
                    preferred_element_type=F32,
                )
            for h in range(2):
                act_part[h, q] = act[h * half_rows : (h + 1) * half_rows]
        send(remote(act_part.at[other], act_in, dense_send.at[2], dense_recv.at[2], across_core))

    def dense_back(r, g):
        arrived(("act",), act_in, dense_send.at[2], dense_recv.at[2])
        lane = iota(act_in.shape[1:], 1)
        for q in range(PLANES):
            act = act_part[tp, q] + act_in[q]
            units = jax.nn.silu(act) * pltpu.roll(act, quarter, 1)
            units = jnp.where(lane < quarter, units, 0.0).astype(BF16)
            if q == 0:
                dense_hid[tp, plane] = units
                continue
            slot = dense_units.at[q]
            slot[...] = units
            send(
                remote(
                    slot, dense_hid.at[tp, plane], back_send.at[q], back_recv.at[plane],
                    place(rounds[q]),
                )
            )

    def dense_pair(r, g):
        for q in range(1, PLANES):
            z = rounds[q]
            arrived(("back", q), dense_hid.at[tp, z], back_send.at[q], back_recv.at[z])
        piece = dense_hid.at[tp]
        send(remote(piece, piece, dense_send.at[3], dense_recv.at[3], across_core))

    def dense_out(r, g):
        arrived(("pair",), dense_hid.at[other], dense_send.at[3], dense_recv.at[3])
        loads[2].wait()
        dense_down_v[pl.ds(dense_depth, quarter)] = jnp.zeros((quarter, half_width), BF16)
        result = 0.0
        for q in range(PLANES):
            units = jnp.concatenate([dense_hid[0, q], dense_hid[1, q]], axis=0)
            result = result + jnp.dot(
                units, dense_down_v[pl.ds(q * quarter, 2 * quarter)], preferred_element_type=F32
            )
        total[...] = jax.nn.sigmoid(branch_ref[...]) * result

    def collect(r, g):
        z = rounds[r]
        for h in range(2):
            mine = 2 * z + (1 - line if h else line)
            if r or h:
                arrived(("ret", r, h), returned.at[mine], ret_send.at[r, h], ret_recv.at[mine])
        kept = (2 * slot_count * z + iota((tok_rows, 2 * slot_count), 1)).astype(F32)
        expert_out = returned[pl.ds(2 * z, 2)].reshape(2 * slot_count, half_width)
        routed = total[...]
        for t in range(top_count):
            picker = (codes[:, t : t + 1] == kept).astype(F32).astype(BF16)
            routed = routed + shares[:, t : t + 1] * jnp.dot(
                picker, expert_out, preferred_element_type=F32
            )
        total[...] = routed

    loaded = []
    steps = dict(
        cross=cross, along=along, take=take, over=over, share=share, expand=expand,
        contract=contract, reduce=reduce, scatter=scatter, spread_x=spread_x,
        spread_y=spread_y, dense_act=dense_act, dense_back=dense_back,
        dense_pair=dense_pair, dense_out=dense_out, collect=collect,
    )
    for name, r, i in PLAN:
        steps[name](r, i)
    out_ref[...] = total[...].astype(BF16)

    for copy, condition in unsent:
        if condition is None:
            copy.wait_send()
        else:
            pl.when(condition)(copy.wait_send)


def per_device(
    tokens,
    expert_ids,
    route_weights,
    norm_gain,
    gate_weight,
    up_weight,
    down_weight,
    dense_gate,
    dense_up,
    dense_down,
    branch_gate,
):
    tok_rows, width = tokens.shape
    top_count = expert_ids.shape[1]
    ep_count = lax.axis_size("ep")
    experts = ep_count // 2
    slot_count = 2 * top_count * tok_rows // experts
    half_width, columns = width // 2, gate_weight.shape[1]
    chunk, units, depth = half_width // OWN_CHUNKS, dense_gate.shape[1], dense_gate.shape[0]
    quarter = units // PLANES
    fits = (
        ep_count == 4 * PLANES
        and tok_rows == 128
        and top_count <= 8
        and slot_count & (slot_count - 1) == 0
        and slot_count % 16 == 0
        and chunk % 128 == 0
        and quarter == 64
        and depth % 16 == 0
    )
    if not fits:
        return small_slot_path(
            tokens, expert_ids, route_weights, norm_gain, gate_weight, up_weight,
            down_weight, dense_gate, dense_up, dense_down, branch_gate,
        )
    parts = OWN_CHUNKS + CROSSED
    dma = pltpu.SemaphoreType.DMA
    vmem = pl.BlockSpec(memory_space=pltpu.VMEM)
    hbm = pl.BlockSpec(memory_space=pl.ANY)
    return pl.pallas_call(
        functools.partial(expert_kernel, (ep_count, experts, slot_count, top_count)),
        out_shape=jax.ShapeDtypeStruct((tok_rows, half_width), BF16),
        in_specs=[vmem] * 4 + [hbm] * 6 + [vmem],
        out_specs=vmem,
        scratch_shapes=[
            pltpu.VMEM((PLANES, parts, tok_rows, chunk), BF16),
            pltpu.VMEM((PLANES, 2, 16, tok_rows), BF16),
            pltpu.VMEM((PLANES, 2, 2, 2, OWN_CHUNKS, slot_count, chunk), BF16),
            pltpu.VMEM((PLANES, parts, slot_count, chunk), BF16),
            pltpu.VMEM((PLANES, 2, 2, 2 * slot_count, columns), BF16),
            pltpu.VMEM((PLANES, 2, 2, slot_count, half_width), BF16),
            pltpu.VMEM((PLANES, 2, slot_count, half_width), BF16),
            pltpu.VMEM((PLANES, 2, slot_count, half_width), BF16),
            pltpu.VMEM((experts, slot_count, half_width), BF16),
            pltpu.VMEM(gate_weight.shape, BF16),
            pltpu.VMEM(up_weight.shape, BF16),
            pltpu.VMEM(down_weight.shape, BF16),
            pltpu.VMEM(dense_gate.shape, BF16),
            pltpu.VMEM(dense_up.shape, BF16),
            pltpu.VMEM((units + quarter, half_width), BF16),
            pltpu.VMEM((PLANES, depth, 2 * quarter), BF16),
            pltpu.VMEM((2, 2, 2, depth, 2 * quarter), BF16),
            pltpu.VMEM((2, PLANES, tok_rows // 2, 2 * quarter), F32),
            pltpu.VMEM((PLANES, tok_rows // 2, 2 * quarter), F32),
            pltpu.VMEM((2, PLANES, tok_rows // 2, 2 * quarter), BF16),
            pltpu.VMEM((PLANES, tok_rows // 2, 2 * quarter), BF16),
            pltpu.VMEM((tok_rows, half_width), F32),
            dma((6,)),
            dma((3, 2 * PLANES)),
            dma((PLANES, 2)),
            dma((PLANES, parts)),
            dma((PLANES, parts)),
            dma((PLANES, parts)),
            dma((max(CROSSED, 1),)),
            dma((max(CROSSED, 1),)),
            dma((PLANES, parts)),
            dma((PLANES, parts)),
            dma((PLANES, OWN_CHUNKS)),
            dma((PLANES, OWN_CHUNKS)),
            dma((PLANES, OWN_CHUNKS)),
            dma((PLANES, OWN_CHUNKS)),
            dma((PLANES, 2)),
            dma((PLANES, 2)),
            dma((PLANES, 2)),
            dma((PLANES, 2)),
            dma((PLANES, 2)),
            dma((PLANES, 2)),
            dma((PLANES, 2)),
            dma((experts,)),
            dma((PLANES,)),
            dma((2,)),
            dma((4,)),
            dma((4,)),
            dma((PLANES,)),
            dma((PLANES,)),
        ],
        compiler_params=pltpu.CompilerParams(
            collective_id=0, has_side_effects=True, vmem_limit_bytes=60000 * 1024
        ),
    )(
        tokens, expert_ids.T, route_weights.T, norm_gain[None, :], gate_weight, up_weight,
        down_weight, dense_gate, dense_up, dense_down, branch_gate[None, :],
    )


def solution(mesh):
    in_specs = (
        P("ep", None),
        P("ep", None),
        P("ep", None),
        P(),
        P(None, ("ep", "tp")),
        P(None, ("ep", "tp")),
        P("ep", "tp"),
        P("ep", None),
        P("ep", None),
        P(None, "tp"),
        P("tp"),
    )
    out_specs = P("ep", "tp")
    return jax.shard_map(
        per_device, mesh=mesh, in_specs=in_specs, out_specs=out_specs, check_vma=False
    )
```

```python
import functools

import jax
import jax.numpy as jnp
from jax import lax
from jax.experimental import pallas as pl
from jax.experimental.pallas import tpu as pltpu
from jax.sharding import PartitionSpec as P

epsilon = 1e-06


def narrowed(rows):
    half_features = rows.shape[2] // 2
    return lax.dynamic_slice_in_dim(rows, lax.axis_index("tp") * half_features, half_features, 2)


def small_slot_path(
    tokens,
    expert_ids,
    route_weights,
    norm_gain,
    gate_weight,
    up_weight,
    down_weight,
    dense_gate,
    dense_up,
    dense_down,
    branch_gate,
):
    tok_rows, model_width = tokens.shape
    top_count = expert_ids.shape[1]
    ep_count = lax.axis_size("ep")
    experts = ep_count // 2
    slot_count = 2 * top_count * tok_rows // experts
    values = tokens.astype(jnp.float32)
    inverse = lax.rsqrt(jnp.mean(values * values, axis=1, keepdims=True) + epsilon)
    normed = (values * inverse * norm_gain[None, :]).astype(jnp.bfloat16)
    dense_gate_act = jnp.dot(
        normed,
        lax.all_gather(dense_gate, "ep", axis=0, tiled=True),
        preferred_element_type=jnp.float32,
    )
    dense_up_act = jnp.dot(
        normed,
        lax.all_gather(dense_up, "ep", axis=0, tiled=True),
        preferred_element_type=jnp.float32,
    )
    dense_hidden = (jax.nn.silu(dense_gate_act) * dense_up_act).astype(jnp.bfloat16)
    dense_out = jnp.dot(dense_hidden, dense_down, preferred_element_type=jnp.float32)
    flat_ids = expert_ids.reshape(tok_rows * top_count)
    labels = lax.broadcasted_iota(jnp.int32, (1, experts), 1)
    onehot = (flat_ids[:, None] == labels).astype(jnp.int32)
    earlier = jnp.cumsum(onehot, axis=0) - onehot
    slot_index = jnp.sum(onehot * earlier, axis=1)
    row_code = (flat_ids * slot_count + slot_index).reshape(tok_rows, top_count)
    targets = lax.broadcasted_iota(jnp.int32, (experts * slot_count, 1, 1), 0)
    selector = jnp.any(row_code[None, :, :] == targets, axis=2).astype(jnp.bfloat16)
    buffer = jnp.dot(selector, normed, preferred_element_type=jnp.float32).astype(jnp.bfloat16)
    buffer = buffer.reshape(experts, slot_count, model_width)
    outgoing = narrowed(jnp.repeat(buffer, 2, axis=0))
    arrived = lax.all_gather(
        lax.all_to_all(outgoing, "ep", split_axis=0, concat_axis=0, tiled=True),
        "tp",
        axis=2,
        tiled=True,
    )
    in_rows = arrived.reshape(ep_count * slot_count, model_width)
    expert_gate = jnp.dot(in_rows, gate_weight, preferred_element_type=jnp.float32)
    expert_up = jnp.dot(in_rows, up_weight, preferred_element_type=jnp.float32)
    hidden = (jax.nn.silu(expert_gate) * expert_up).astype(jnp.bfloat16)
    down_total = jnp.dot(
        lax.all_gather(hidden, "tp", axis=1, tiled=True),
        down_weight,
        preferred_element_type=jnp.float32,
    )
    partial_value = down_total.astype(jnp.bfloat16).reshape(ep_count, slot_count, -1)
    returned_rows = lax.all_to_all(partial_value, "ep", split_axis=0, concat_axis=0, tiled=True)
    pair_sums = returned_rows.reshape(experts, 2, slot_count, -1).astype(jnp.float32)
    expert_out = (
        (pair_sums[:, 0] + pair_sums[:, 1]).astype(jnp.bfloat16).reshape(experts * slot_count, -1)
    )
    picked = (
        jnp.take(expert_out, row_code.reshape(-1), axis=0)
        .reshape(tok_rows, top_count, -1)
        .astype(jnp.float32)
    )
    routed = jnp.sum(route_weights[:, :, None] * picked, axis=1)
    mixed_out = routed + jax.nn.sigmoid(branch_gate)[None, :] * dense_out
    return mixed_out.astype(jnp.bfloat16)


MESH = pl.DeviceIdType.MESH
BF16, F32 = jnp.bfloat16, jnp.float32


def flip(value, bits):
    bit = 1
    while bit <= bits:
        if bits & bit:
            value = value + bit * (1 - 2 * lax.rem(lax.div(value, bit), 2))
        bit *= 2
    return value


PLANES, OWN_CHUNKS, CROSSED, PIECES = 4, 2, 1, 2
PLAN = (
    ("scatter", 0, 0),
    ("scatter", 0, 3),
    ("cross", 0, 0),
    ("take", 0, 0),
    ("take", 0, 1),
    ("scatter", 0, 2),
    ("along", 0, 0),
    ("along", 0, 1),
    ("take", 0, 2),
    ("scatter", 0, 1),
    ("along", 0, 2),
    ("over", 0, 0),
    ("take", 1, 0),
    ("along", 2, 0),
    ("share_own", 0, 1),
    ("share_own", 0, 0),
    ("take", 2, 0),
    ("along", 2, 1),
    ("along", 1, 0),
    ("spread_x", 0, 0),
    ("share_far", 0, 1),
    ("share_far", 0, 0),
    ("along", 1, 1),
    ("take", 1, 1),
    ("share_own", 1, 0),
    ("over", 1, 0),
    ("take", 2, 1),
    ("expand", 0, 1),
    ("take", 1, 2),
    ("over", 2, 0),
    ("along", 2, 2),
    ("along", 1, 2),
    ("share_far", 1, 0),
    ("take", 2, 2),
    ("share_own", 2, 0),
    ("share_far", 2, 0),
    ("contract", 0, 2),
    ("expand", 2, 0),
    ("share_own", 1, 1),
    ("take", 3, 0),
    ("along", 3, 0),
    ("expand", 1, 0),
    ("share_own", 2, 1),
    ("contract", 2, 0),
    ("spread_y", 0, 0),
    ("contract", 2, 1),
    ("take", 3, 1),
    ("share_far", 2, 1),
    ("contract", 1, 0),
    ("expand", 0, 0),
    ("along", 3, 1),
    ("share_far", 1, 1),
    ("expand", 2, 1),
    ("over", 3, 0),
    ("reduce", 2, 0),
    ("take", 3, 2),
    ("expand", 1, 1),
    ("share_far", 3, 0),
    ("share_own", 3, 0),
    ("contract", 2, 2),
    ("reduce", 0, 2),
    ("reduce", 2, 1),
    ("contract", 0, 3),
    ("along", 3, 2),
    ("dense_act", 0, 0),
    ("share_own", 3, 1),
    ("expand", 3, 0),
    ("share_far", 3, 1),
    ("dense_back", 0, 0),
    ("contract", 1, 1),
    ("contract", 3, 0),
    ("expand", 3, 1),
    ("reduce", 1, 0),
    ("reduce", 2, 2),
    ("reduce", 0, 3),
    ("contract", 3, 2),
    ("contract", 3, 3),
    ("contract", 1, 2),
    ("contract", 3, 1),
    ("reduce", 1, 1),
    ("contract", 1, 3),
    ("contract", 2, 3),
    ("reduce", 3, 0),
    ("reduce", 3, 2),
    ("reduce", 3, 3),
    ("reduce", 1, 2),
    ("dense_pair", 0, 0),
    ("dense_out", 0, 0),
    ("collect", 2, 0),
    ("reduce", 3, 1),
    ("contract", 0, 0),
    ("contract", 0, 1),
    ("reduce", 1, 3),
    ("reduce", 2, 3),
    ("collect", 1, 0),
    ("reduce", 0, 0),
    ("collect", 0, 0),
    ("collect", 2, 1),
    ("collect", 1, 1),
    ("collect", 3, 0),
    ("reduce", 0, 1),
    ("collect", 0, 1),
    ("collect", 3, 1),
)


def expert_kernel(
    dims,
    tokens_ref,
    ids_ref,
    route_ref,
    gain_ref,
    gate_hbm,
    up_hbm,
    down_hbm,
    dense_gate_hbm,
    dense_up_hbm,
    dense_down_hbm,
    branch_ref,
    out_ref,
    blocks,
    meta,
    rows_in,
    row_send,
    hidden,
    half_own,
    half_in,
    summed,
    returned,
    gate_w,
    up_w,
    down_w,
    dense_gate_v,
    dense_up_v,
    dense_down_v,
    slices,
    dense_w,
    act_part,
    act_in,
    dense_hid,
    dense_units,
    total,
    load_sem,
    meta_send,
    meta_recv,
    along_send,
    block_recv,
    cross_send,
    cross_recv,
    y_send,
    y_recv,
    x_send,
    x_recv,
    xy_send,
    xy_recv,
    core_send,
    core_recv,
    hid_send,
    hid_recv,
    half_send,
    half_recv,
    ret_send,
    ret_recv,
    slice_send,
    slice_recv,
    dense_send,
    dense_recv,
    back_send,
    back_recv,
):
    ep_count, experts, slot_count, top_count = dims
    tok_rows = tokens_ref.shape[0]
    chunk = blocks.shape[3]
    half_width = chunk * OWN_CHUNKS
    piece_width = half_width // PIECES
    quarter = dense_gate_v.shape[1] // PLANES
    ep, tp = lax.axis_index("ep"), lax.axis_index("tp")
    other = 1 - tp
    side, line, plane = lax.rem(ep, 2), lax.rem(lax.div(ep, 2), 2), lax.div(ep, 4)
    inner = lax.rem(lax.div(plane + 1, 2), 2)
    near, far = flip(plane, 2), flip(plane, 3)
    rounds = [plane, flip(plane, 1), near + inner * (far - near), far + inner * (near - far)]

    def place(to_plane, to_line=None, to_side=None, core=None):
        to_line = line if to_line is None else to_line
        to_side = side if to_side is None else to_side
        return (4 * to_plane + 2 * to_line + to_side, tp if core is None else core)

    across_x = place(plane, None, 1 - side)
    across_y = place(plane, 1 - line)
    across_core = place(plane, None, None, other)

    def remote(src, dst, send, recv, device):
        return pltpu.make_async_remote_copy(
            src_ref=src, dst_ref=dst, send_sem=send, recv_sem=recv,
            device_id=device, device_id_type=MESH,
        )

    barrier = pltpu.get_barrier_semaphore()

    rises, falls = plane < PLANES - 1, plane > 0
    above, below = jnp.minimum(plane + 1, PLANES - 1), jnp.maximum(plane - 1, 0)
    greeted = [across_x, across_core, across_y]
    for other_plane in rounds[1:]:
        greeted += [place(other_plane), place(other_plane, 1 - line)]
    for device in greeted:
        pl.semaphore_signal(barrier, inc=1, device_id=device, device_id_type=MESH)

    dense_depth = dense_down_hbm.shape[0]
    loads = [
        pltpu.make_async_copy(source, target, load_sem.at[i])
        for i, (source, target) in enumerate(
            (
                (dense_gate_hbm, dense_gate_v),
                (dense_up_hbm, dense_up_v),
                (dense_down_hbm, dense_down_v.at[pl.ds(0, dense_depth)]),
                (gate_hbm, gate_w),
                (up_hbm, up_w),
                (down_hbm, down_w),
            )
        )
    ]
    for load in loads:
        load.start()

    values = tokens_ref[...].astype(F32)
    inverse = lax.rsqrt(jnp.mean(values * values, axis=1, keepdims=True) + epsilon)
    for i in range(OWN_CHUNKS):
        columns = pl.ds(pl.multiple_of(tp * half_width + i * chunk, chunk), chunk)
        blocks[plane, i] = (
            tokens_ref[:, columns].astype(F32) * inverse * gain_ref[:, columns]
        ).astype(BF16)

    def iota(shape, axis):
        return lax.broadcasted_iota(jnp.int32, shape, axis)

    label_rows = max(experts, 16)
    labels = iota((label_rows, tok_rows), 0)
    hits = [ids_ref[t : t + 1, :] == labels for t in range(top_count)]
    named = sum(hit.astype(F32) for hit in hits).astype(BF16)
    before = (iota((tok_rows, tok_rows), 0) < iota((tok_rows, tok_rows), 1)).astype(F32)
    earlier = jnp.dot(named, before.astype(BF16), preferred_element_type=F32)
    meta_rows = iota((meta.shape[2], tok_rows), 0)
    code_rows = iota((8, tok_rows), 0)
    listed = jnp.zeros(meta_rows.shape, F32)
    coded = jnp.zeros(code_rows.shape, F32)
    for t in range(top_count):
        expert = ids_ref[t : t + 1, :].astype(F32)
        slot = jnp.sum(jnp.where(hits[t], earlier, 0.0), axis=0, keepdims=True)
        listed = jnp.where(meta_rows == 2 * t, expert, listed)
        listed = jnp.where(meta_rows == 2 * t + 1, slot, listed)
        coded = jnp.where(code_rows == t, expert * slot_count + slot, coded)
    meta[plane, 0] = listed.astype(BF16)
    codes = jnp.transpose(coded)
    shares = jnp.transpose(route_ref[...])

    pl.semaphore_wait(barrier, len(greeted))

    unsent, lanes = [], {}

    def send(copy, condition=None, lane=None):
        if lane is None:
            unsent.append((copy, condition))
        else:
            if lane in lanes:
                lanes[lane].wait_send()
            lanes[lane] = copy
        if condition is None:
            copy.start()
        else:
            pl.when(condition)(copy.start)

    seen = set()

    def arrived(key, ref, send_sem, recv_sem, condition=None):
        if key in seen:
            return
        seen.add(key)
        copy = remote(ref, ref, send_sem, recv_sem, across_core)
        if condition is None:
            copy.wait_recv()
        else:
            pl.when(condition)(copy.wait_recv)

    plain = OWN_CHUNKS - CROSSED
    parts = OWN_CHUNKS + CROSSED

    def belongs(i):
        return (0, i) if i < OWN_CHUNKS else (1, i - CROSSED)

    def cross(_, j):
        if j == 0:
            send(
                remote(
                    meta.at[plane, 0], meta.at[plane, 1],
                    cross_send.at[CROSSED], meta_recv.at[plane, 1], across_x,
                )
            )
        send(
            remote(
                blocks.at[plane, plain + j], blocks.at[plane, OWN_CHUNKS + j],
                cross_send.at[j], cross_recv.at[j], across_x,
            )
        )

    def have(r, i):
        z = rounds[r]
        if r == 0:
            if i >= OWN_CHUNKS:
                arrived(("meta", r, 1), meta.at[z, 1], cross_send.at[CROSSED], meta_recv.at[z, 1])
                j = i - OWN_CHUNKS
                arrived(("cross", j), blocks.at[z, i], cross_send.at[j], cross_recv.at[j])
            return
        of = belongs(i)[0]
        arrived(("meta", r, of), meta.at[z, of], cross_send.at[CROSSED], meta_recv.at[z, of])
        arrived(("block", r, i), blocks.at[z, i], along_send.at[r, i], block_recv.at[z, i])

    def along(r, i):
        have(r, i)
        z = rounds[r]
        of = belongs(i)[0]
        first = i in (0, OWN_CHUNKS)
        ways = (
            ((z <= plane) & rises, above, r),
            ((z >= plane) & falls, below, r or PLANES),
        )
        for condition, target, way in ways:
            if first:
                piece = meta.at[z, of]
                send(
                    remote(
                        piece, piece, meta_send.at[of, way], meta_recv.at[z, of], place(target)
                    ),
                    condition,
                )
            piece = blocks.at[z, i]
            send(
                remote(piece, piece, along_send.at[way, i], block_recv.at[z, i], place(target)),
                condition,
            )

    pick_row = iota((2 * slot_count, tok_rows), 0)
    pick_expert = (
        2 * plane + jnp.where(pick_row < slot_count, line, 1 - line)
    ).astype(F32)
    pick_slot = jnp.bitwise_and(pick_row, slot_count - 1).astype(F32)

    def take(r, i):
        have(r, i)
        z = rounds[r]
        of, c = belongs(i)
        listing = meta[z, of].astype(F32)
        chosen = sum(
            (
                (listing[2 * t : 2 * t + 1] == pick_expert)
                & (listing[2 * t + 1 : 2 * t + 2] == pick_slot)
            ).astype(F32)
            for t in range(top_count)
        ).astype(BF16)
        picked = jnp.dot(chosen, blocks[z, i], preferred_element_type=F32).astype(BF16)
        rows_in[z, 0, tp, of, c] = picked[:slot_count]
        row_send[r, i] = picked[slot_count:]
        send(
            remote(
                row_send.at[r, i], rows_in.at[z, 1, tp, of, c],
                y_send.at[r, i], y_recv.at[z, i], across_y,
            ),
        )
        if i < plain:
            send(
                remote(
                    rows_in.at[z, 0, tp, 0, i], rows_in.at[z, 0, tp, 1, i],
                    x_send.at[r, i], x_recv.at[z, i], across_x,
                )
            )

    def have_line(r, i):
        of, c = belongs(i)
        z = rounds[r]
        arrived(("y", r, i), rows_in.at[z, 1, tp, of, c], y_send.at[r, i], y_recv.at[z, i])

    def over(r, i):
        have_line(r, i)
        z = rounds[r]
        send(
            remote(
                rows_in.at[z, 1, tp, 0, i], rows_in.at[z, 1, tp, 1, i],
                xy_send.at[r, i], xy_recv.at[z, i], across_x,
            )
        )

    def pass_rows(r, g, of):
        piece = rows_in.at[rounds[r], g, tp, of]
        send(
            remote(
                piece, piece, core_send.at[r, g, of], core_recv.at[rounds[r], g, of], across_core
            ),
        )

    def share_own(r, g):
        if g:
            for i in range(OWN_CHUNKS):
                have_line(r, i)
        pass_rows(r, g, 0)

    def share_far(r, g):
        z = rounds[r]
        if g:
            for i in range(OWN_CHUNKS, parts):
                have_line(r, i)
        sems = ((x_send, x_recv), (xy_send, xy_recv))[g]
        for i in range(plain):
            arrived(
                ("x", r, g, i), rows_in.at[z, g, tp, 1, i], sems[0].at[r, i], sems[1].at[z, i]
            )
        pass_rows(r, g, 1)

    def expand(r, g):
        z = rounds[r]
        for of in range(2):
            arrived(
                ("core", r, g, of), rows_in.at[z, g, other, of],
                core_send.at[r, g, of], core_recv.at[z, g, of],
            )
        if not loaded:
            for load in loads[3:]:
                load.wait()
            loaded.append(True)
        gate, up = 0.0, 0.0
        for core in range(2):
            for c in range(OWN_CHUNKS):
                rows = rows_in[z, g, core, :, c].reshape(2 * slot_count, chunk)
                depth = pl.ds((core * OWN_CHUNKS + c) * chunk, chunk)
                gate = gate + jnp.dot(rows, gate_w[depth, :], preferred_element_type=F32)
                up = up + jnp.dot(rows, up_w[depth, :], preferred_element_type=F32)
        hidden[z, g, tp] = (jax.nn.silu(gate) * up).astype(BF16)
        piece = hidden.at[z, g, tp]
        send(
            remote(piece, piece, hid_send.at[g], hid_recv.at[z, g], across_core),
            lane=("hid", g),
        )

    def contract(r, i):
        z = rounds[r]
        g, p = i // PIECES, i % PIECES
        arrived(("hid", r, g), hidden.at[z, g, other], hid_send.at[g], hid_recv.at[z, g])
        units = jnp.concatenate([hidden[z, g, 0], hidden[z, g, 1]], axis=1)
        half_own[r, i] = (
            jnp.dot(
                units, down_w[:, p * piece_width : (p + 1) * piece_width],
                preferred_element_type=F32,
            )
            .astype(BF16)
            .reshape(2, slot_count, piece_width)
        )
        send(
            remote(
                half_own.at[r, i, 1], half_in.at[z, i],
                half_send.at[r, i], half_recv.at[z, i], across_x,
            )
        )

    def reduce(r, i):
        z = rounds[r]
        g, p = i // PIECES, i % PIECES
        arrived(("half", r, i), half_in.at[z, i], half_send.at[r, i], half_recv.at[z, i])
        result = (half_own[r, i, 0].astype(F32) + half_in[z, i].astype(F32)).astype(BF16)
        mine = 2 * plane + line
        if r == 0 and g == 0:
            returned[p, mine] = result
            return
        summed[r, i] = result
        target = place(z, 1 - line if g else line)
        send(
            remote(
                summed.at[r, i], returned.at[p, mine],
                ret_send.at[r, i], ret_recv.at[p, mine], target,
            )
        )

    half_plane = lax.rem(plane, 2)
    feeds = tp == lax.div(plane, 2)

    def scatter(_, q):
        if q:
            z = rounds[q]
            send(
                remote(
                    slices.at[z], dense_w.at[line, side, half_plane],
                    slice_send.at[q], slice_recv.at[half_plane], place(z),
                ),
                feeds,
            )
            return
        loads[0].wait()
        loads[1].wait()
        lane = iota((dense_gate_v.shape[0], 2 * quarter), 1)
        for q in range(PLANES):
            columns = pl.ds((q // 2) * 2 * quarter, 2 * quarter)
            gate = dense_gate_v[:, columns].astype(F32)
            up = dense_up_v[:, columns].astype(F32)
            if q % 2:
                gate = pltpu.roll(gate, quarter, 1)
            else:
                up = pltpu.roll(up, quarter, 1)
            slices[q] = jnp.where(lane < quarter, gate, up).astype(BF16)

        @pl.when(feeds)
        def _():
            dense_w[line, side, half_plane] = slices[plane]

    def spread_x(r, g):
        for h in range(2):
            arrived(
                ("slice", h), dense_w.at[line, side, h], slice_send.at[1], slice_recv.at[h],
                2 * tp + h != plane,
            )
        piece = dense_w.at[line, side]
        send(remote(piece, piece, dense_send.at[0], dense_recv.at[0], across_x))

    def spread_y(r, g):
        arrived(("wx",), dense_w.at[line, 1 - side], dense_send.at[0], dense_recv.at[0])
        piece = dense_w.at[line]
        send(remote(piece, piece, dense_send.at[1], dense_recv.at[1], across_y))

    def dense_act(r, g):
        arrived(("wy",), dense_w.at[1 - line], dense_send.at[1], dense_recv.at[1])
        weights = jnp.concatenate(
            [dense_w[l, s, h] for h in range(2) for l in range(2) for s in range(2)], axis=0
        )
        half_rows = tok_rows // 2
        for q in range(PLANES):
            act = 0.0
            for i in range(OWN_CHUNKS):
                have(q, i)
                act = act + jnp.dot(
                    blocks[rounds[q], i], weights[i * chunk : (i + 1) * chunk],
                    preferred_element_type=F32,
                )
            for h in range(2):
                act_part[h, q] = act[h * half_rows : (h + 1) * half_rows]
        send(remote(act_part.at[other], act_in, dense_send.at[2], dense_recv.at[2], across_core))

    def dense_back(r, g):
        arrived(("act",), act_in, dense_send.at[2], dense_recv.at[2])
        lane = iota(act_in.shape[1:], 1)
        for q in range(PLANES):
            act = act_part[tp, q] + act_in[q]
            units = jax.nn.silu(act) * pltpu.roll(act, quarter, 1)
            units = jnp.where(lane < quarter, units, 0.0).astype(BF16)
            if q == 0:
                dense_hid[tp, plane] = units
                continue
            slot = dense_units.at[q]
            slot[...] = units
            send(
                remote(
                    slot, dense_hid.at[tp, plane], back_send.at[q], back_recv.at[plane],
                    place(rounds[q]),
                )
            )

    def dense_pair(r, g):
        for q in range(1, PLANES):
            z = rounds[q]
            arrived(("back", q), dense_hid.at[tp, z], back_send.at[q], back_recv.at[z])
        piece = dense_hid.at[tp]
        send(remote(piece, piece, dense_send.at[3], dense_recv.at[3], across_core))

    def dense_out(r, g):
        arrived(("pair",), dense_hid.at[other], dense_send.at[3], dense_recv.at[3])
        loads[2].wait()
        dense_down_v[pl.ds(dense_depth, quarter)] = jnp.zeros((quarter, half_width), BF16)
        result = 0.0
        for q in range(PLANES):
            units = jnp.concatenate([dense_hid[0, q], dense_hid[1, q]], axis=0)
            result = result + jnp.dot(
                units, dense_down_v[pl.ds(q * quarter, 2 * quarter)], preferred_element_type=F32
            )
        total[...] = jax.nn.sigmoid(branch_ref[...]) * result

    left = [PLANES] * PIECES

    def collect(r, p):
        z = rounds[r]
        for h in range(2):
            mine = 2 * z + (1 - line if h else line)
            if r or h:
                arrived(
                    ("ret", r, h, p), returned.at[p, mine],
                    ret_send.at[r, PIECES * h + p], ret_recv.at[p, mine],
                )
        kept = (2 * slot_count * z + iota((tok_rows, 2 * slot_count), 1)).astype(F32)
        expert_out = returned[p, pl.ds(2 * z, 2)].reshape(2 * slot_count, piece_width)
        columns = slice(p * piece_width, (p + 1) * piece_width)
        routed = total[:, columns]
        for t in range(top_count):
            picker = (codes[:, t : t + 1] == kept).astype(F32).astype(BF16)
            routed = routed + shares[:, t : t + 1] * jnp.dot(
                picker, expert_out, preferred_element_type=F32
            )
        left[p] -= 1
        if left[p]:
            total[:, columns] = routed
        else:
            out_ref[:, columns] = routed.astype(BF16)

    loaded = []
    steps = dict(
        cross=cross, along=along, take=take, over=over, share_own=share_own, share_far=share_far, expand=expand,
        contract=contract, reduce=reduce, scatter=scatter, spread_x=spread_x,
        spread_y=spread_y, dense_act=dense_act, dense_back=dense_back,
        dense_pair=dense_pair, dense_out=dense_out, collect=collect,
    )
    for name, r, i in PLAN:
        steps[name](r, i)

    for copy in lanes.values():
        copy.wait_send()
    for copy, condition in unsent:
        if condition is None:
            copy.wait_send()
        else:
            pl.when(condition)(copy.wait_send)


def per_device(
    tokens,
    expert_ids,
    route_weights,
    norm_gain,
    gate_weight,
    up_weight,
    down_weight,
    dense_gate,
    dense_up,
    dense_down,
    branch_gate,
):
    tok_rows, width = tokens.shape
    top_count = expert_ids.shape[1]
    ep_count = lax.axis_size("ep")
    experts = ep_count // 2
    slot_count = 2 * top_count * tok_rows // experts
    half_width, columns = width // 2, gate_weight.shape[1]
    chunk, units, depth = half_width // OWN_CHUNKS, dense_gate.shape[1], dense_gate.shape[0]
    quarter = units // PLANES
    fits = (
        ep_count == 4 * PLANES
        and tok_rows == 128
        and top_count <= 8
        and slot_count & (slot_count - 1) == 0
        and slot_count % 16 == 0
        and chunk % 128 == 0
        and half_width % (128 * PIECES) == 0
        and quarter == 64
        and depth % 16 == 0
    )
    if not fits:
        return small_slot_path(
            tokens, expert_ids, route_weights, norm_gain, gate_weight, up_weight,
            down_weight, dense_gate, dense_up, dense_down, branch_gate,
        )
    parts, plain = OWN_CHUNKS + CROSSED, OWN_CHUNKS - CROSSED
    dma = pltpu.SemaphoreType.DMA
    vmem = pl.BlockSpec(memory_space=pltpu.VMEM)
    hbm = pl.BlockSpec(memory_space=pl.ANY)
    return pl.pallas_call(
        functools.partial(expert_kernel, (ep_count, experts, slot_count, top_count)),
        out_shape=jax.ShapeDtypeStruct((tok_rows, half_width), BF16),
        in_specs=[vmem] * 4 + [hbm] * 6 + [vmem],
        out_specs=vmem,
        scratch_shapes=[
            pltpu.VMEM((PLANES, parts, tok_rows, chunk), BF16),
            pltpu.VMEM((PLANES, 2, 16, tok_rows), BF16),
            pltpu.VMEM((PLANES, 2, 2, 2, OWN_CHUNKS, slot_count, chunk), BF16),
            pltpu.VMEM((PLANES, parts, slot_count, chunk), BF16),
            pltpu.VMEM((PLANES, 2, 2, 2 * slot_count, columns), BF16),
            pltpu.VMEM((PLANES, 2 * PIECES, 2, slot_count, half_width // PIECES), BF16),
            pltpu.VMEM((PLANES, 2 * PIECES, slot_count, half_width // PIECES), BF16),
            pltpu.VMEM((PLANES, 2 * PIECES, slot_count, half_width // PIECES), BF16),
            pltpu.VMEM((PIECES, experts, slot_count, half_width // PIECES), BF16),
            pltpu.VMEM(gate_weight.shape, BF16),
            pltpu.VMEM(up_weight.shape, BF16),
            pltpu.VMEM(down_weight.shape, BF16),
            pltpu.VMEM(dense_gate.shape, BF16),
            pltpu.VMEM(dense_up.shape, BF16),
            pltpu.VMEM((units + quarter, half_width), BF16),
            pltpu.VMEM((PLANES, depth, 2 * quarter), BF16),
            pltpu.VMEM((2, 2, 2, depth, 2 * quarter), BF16),
            pltpu.VMEM((2, PLANES, tok_rows // 2, 2 * quarter), F32),
            pltpu.VMEM((PLANES, tok_rows // 2, 2 * quarter), F32),
            pltpu.VMEM((2, PLANES, tok_rows // 2, 2 * quarter), BF16),
            pltpu.VMEM((PLANES, tok_rows // 2, 2 * quarter), BF16),
            pltpu.VMEM((tok_rows, half_width), F32),
            dma((6,)),
            dma((2, PLANES + 1)),
            dma((PLANES, 2)),
            dma((PLANES + 1, parts)),
            dma((PLANES, parts)),
            dma((CROSSED + 1,)),
            dma((CROSSED,)),
            dma((PLANES, parts)),
            dma((PLANES, parts)),
            dma((PLANES, plain)),
            dma((PLANES, plain)),
            dma((PLANES, plain)),
            dma((PLANES, plain)),
            dma((PLANES, 2, 2)),
            dma((PLANES, 2, 2)),
            dma((2,)),
            dma((PLANES, 2)),
            dma((PLANES, 2 * PIECES)),
            dma((PLANES, 2 * PIECES)),
            dma((PLANES, 2 * PIECES)),
            dma((PIECES, experts)),
            dma((PLANES,)),
            dma((2,)),
            dma((4,)),
            dma((4,)),
            dma((PLANES,)),
            dma((PLANES,)),
        ],
        compiler_params=pltpu.CompilerParams(
            collective_id=0, has_side_effects=True, vmem_limit_bytes=60000 * 1024
        ),
    )(
        tokens, expert_ids.T, route_weights.T, norm_gain[None, :], gate_weight, up_weight,
        down_weight, dense_gate, dense_up, dense_down, branch_gate[None, :],
    )


def solution(mesh):
    in_specs = (
        P("ep", None),
        P("ep", None),
        P("ep", None),
        P(),
        P(None, ("ep", "tp")),
        P(None, ("ep", "tp")),
        P("ep", "tp"),
        P("ep", None),
        P("ep", None),
        P(None, "tp"),
        P("tp"),
    )
    out_specs = P("ep", "tp")
    return jax.shard_map(
        per_device, mesh=mesh, in_specs=in_specs, out_specs=out_specs, check_vma=False
    )
```
